32 devices in a mesh: tp: 8 (over z, y), dp: 4 (over x, core).
Axes of the slice: x: 2, y: 2, z: 4, core: 2. Of those that a mesh axis runs over, the one named last changes fastest.
Arguments:
- tokens: bfloat16 [64, 4096], P('tp', 'dp'), may hold values from -30 to 30
- lengths: int32 [64], P('dp'), may hold values from 1 to 2048, 16384 in all
- states: float32 [2, 64, 2048, 128], P(None, 'dp', 'tp'), may hold values from -0.8 to 0.8
- norm_gain: bfloat16 [2, 4096], P(None, 'dp'), may hold values from 0.099609375 to 1.8984375
- w_query: bfloat16 [2, 4096, 2048], P(None, 'dp', 'tp'), may hold values from -0.09375 to 0.09375
- w_key: bfloat16 [2, 4096, 2048], P(None, 'dp', 'tp'), may hold values from -0.09375 to 0.09375
- w_value: bfloat16 [2, 4096, 2048], P(None, 'dp', 'tp'), may hold values from -0.09375 to 0.09375
- w_gate: bfloat16 [2, 4096, 2048], P(None, 'dp', 'tp'), may hold values from -0.09375 to 0.09375
- head_gain: bfloat16 [2, 2048], P(None, 'tp'), may hold values from 0.099609375 to 1.8984375
- w_out: bfloat16 [2, 2048, 4096], P(None, 'tp', 'dp'), may hold values from -0.125 to 0.125
Outputs:
- hidden_out: bfloat16 [64, 4096], P('tp', 'dp')
- new_states: float32 [2, 64, 2048, 128], P(None, 'dp', 'tp')
The draws below stay inside these ranges and needn't reach their ends.
All inputs are finite; a program needn't handle non-finite values. No bound on the sum of `lengths` on one device may be relied on, other than what follows from the above.
Results may differ from the reference program's by a relative error of at most 0.012.
Values may be sent and summed in bfloat16 or wider, within the bound.
No kernel may reach another device: no remote copies, remote signals or barrier semaphores. Data moves between devices by JAX's collectives and lax.ppermute only.
A program may use at most 64 MiB of HBM per device.

```python
import math
import jax
import jax.numpy as jnp
import numpy as np
from jax import lax

D = 4096
HEADS = 16
DK = 128
LAYERS = 2
SEQS = 64


def draw_tokens(key, part):
    key_base, key_rough = jax.random.split(jax.random.fold_in(key, 11), 2)
    base_draw = jax.random.normal(key_base, (SEQS, D), jnp.float32)
    column = jnp.arange(D, dtype=jnp.float32) / (D - 1)
    rough = jax.random.uniform(key_rough, (D,), jnp.float32, 0.5, 1.5)
    column_scale = jnp.exp(math.log(3.0) * column) * rough
    result = base_draw * column_scale[None, :]
    return jnp.clip(result, -30.0, 30.0).astype(jnp.bfloat16)


def block_scale(key, shape, pieces, smallest, high):
    level = 1.0
    for axis_at, blocks in pieces:
        steps = jax.random.uniform(jax.random.fold_in(jax.random.fold_in(key, 6), axis_at), (blocks,), jnp.float32, smallest / len(pieces), high / len(pieces))
        level = level * jnp.repeat(jnp.exp(steps), shape[axis_at] // blocks).reshape((-1,) + (1,) * (len(shape) - 1 - axis_at))
    return level


def profile(number_of, total, limit, skew):
    loads = [(1 << 20) // math.isqrt(standing ** skew) + 1 for standing in range(2, number_of + 1)]
    spare, counts = total - limit - (number_of - 1), [1] * (number_of - 1)
    while spare > 0:
        candidates = [i for i in range(number_of - 1) if counts[i] < limit]
        mass, remaining = sum([loads[i] for i in candidates]), spare
        for i in candidates:
            addition = min(limit - counts[i], max(1, remaining * loads[i] // mass), spare)
            counts[i] = counts[i] + addition
            spare = spare - addition
    return np.array([limit] + counts)


def uneven(key, count, total, most, slope):
    if count == 2:
        one = jax.random.randint(key, (), max(1, total - most), min(most, total - 1) + 1)
        return jnp.stack([one, total - one])
    tallies = jnp.asarray(profile(count, total, most, slope), jnp.int32)
    couples = (count - 1) // 2
    source_of, sink = tallies[1:1 + 2 * couples:2], tallies[2:2 + 2 * couples:2]
    slack = jnp.minimum(source_of - 1, most - sink)
    moved = jax.random.randint(jax.random.fold_in(key, 1), (couples,), 0, 1 << 20) % (slack + 1)
    tallies = tallies.at[1:1 + 2 * couples:2].set(source_of - moved).at[2:2 + 2 * couples:2].set(sink + moved)
    return tallies[jax.random.permutation(jax.random.fold_in(key, 2), count)]


def scatter_about(rng, extent, width, reach, shards=(), kind=jnp.bfloat16):
    values = jax.random.normal(rng, extent, jnp.float32) * width
    if len(shards) > 0:
        values = block_scale(rng, extent, shards, -0.22, 0.18) * values
    return jnp.clip(values, min=-reach, max=reach).astype(kind)


def setup_inputs(seed: int = 0) -> dict:
    key_of = jax.random.split(jax.random.key(seed), 11)
    return {
        "tokens": draw_tokens(jax.random.fold_in(key_of[10], 71), 0),
        "lengths": uneven(key_of[1], SEQS, SEQS * 256, 2048, 2).astype(jnp.int32),
        "states": scatter_about(key_of[2], (LAYERS, SEQS, HEADS * DK, DK), 0.1, 0.8, ((1, 4), (2, 8)), jnp.float32),
        "norm_gain": jnp.clip(1.0 + 0.18 * jax.random.normal(key_of[3], (LAYERS, D), jnp.float32), 0.099609375, 1.8984375).astype(jnp.bfloat16),
        "w_query": scatter_about(key_of[4], (LAYERS, D, HEADS * DK), D ** -0.5, 0.09375, ((1, 4), (2, 8))),
        "w_key": scatter_about(key_of[5], (LAYERS, D, HEADS * DK), D ** -0.5, 0.09375, ((1, 4), (2, 8))),
        "w_value": scatter_about(key_of[6], (LAYERS, D, HEADS * DK), D ** -0.5, 0.09375, ((1, 4), (2, 8))),
        "w_gate": scatter_about(key_of[7], (LAYERS, D, HEADS * DK), D ** -0.5, 0.09375, ((1, 4), (2, 8))),
        "head_gain": jnp.clip(1.0 + 0.18 * jax.random.normal(key_of[8], (LAYERS, HEADS * DK), jnp.float32), 0.099609375, 1.8984375).astype(jnp.bfloat16),
        "w_out": scatter_about(key_of[9], (LAYERS, HEADS * DK, D), (HEADS * DK) ** -0.5, 0.125, ((1, 8), (2, 4))),
    }


norm_eps = 1e-06
group_eps = 1e-05
rotary_base = 10000.0

def rotate(values, positions):
    half_size = values.shape[-1] // 2
    inverse = rotary_base ** (-jnp.arange(half_size, dtype=jnp.float32) / half_size)
    angles = positions.astype(jnp.float32)[:, None] * inverse[None, :]
    cosine = jnp.cos(angles)[:, None, :]
    sine_v = jnp.sin(angles)[:, None, :]
    first_part = values[..., :half_size]
    second = values[..., half_size:]
    return jnp.concatenate([first_part * cosine - second * sine_v, first_part * sine_v + second * cosine], axis=-1)

def decays(head_ids):
    return 1.0 - jnp.exp2(-1.0 - 9.0 * head_ids.astype(jnp.float32) / (HEADS - 1))

def reference(tokens, lengths, states, norm_gain, w_query, w_key, w_value, w_gate, head_gain, w_out):
    batch_size = tokens.shape[0]
    full_width = HEADS * DK
    gammas = decays(jnp.arange(HEADS, dtype=jnp.int32))
    hidden_x = tokens
    outputs = []
    for layer_id in range(LAYERS):
        xfloat = hidden_x.astype(jnp.float32)
        row_scale = lax.rsqrt(lax.optimization_barrier(jnp.sum(xfloat * xfloat, axis=1)) / D + norm_eps)
        normed = (xfloat * norm_gain[layer_id].astype(jnp.float32)).astype(jnp.bfloat16)

        def project(weight):
            product = jnp.dot(normed, weight[layer_id], preferred_element_type=jnp.float32)
            return (product * row_scale[:, None]).astype(jnp.bfloat16)
        query_rows = rotate(project(w_query).astype(jnp.float32).reshape(batch_size, HEADS, DK), lengths)
        key_rows = rotate(project(w_key).astype(jnp.float32).reshape(batch_size, HEADS, DK), lengths) * DK ** (-0.5)
        values_f = project(w_value).astype(jnp.float32).reshape(batch_size, HEADS, DK)
        gate_rows = project(w_gate).astype(jnp.float32)
        prior_state = states[layer_id].reshape(batch_size, HEADS, DK, DK)
        updated = gammas[None, :, None, None] * prior_state + jnp.einsum('bhd,bhv->bhvd', key_rows, values_f)
        readout = jnp.einsum('bhd,bhvd->bhv', query_rows, updated)
        mean_v = lax.optimization_barrier(jnp.mean(readout, axis=-1, keepdims=True))
        square = lax.optimization_barrier(jnp.mean(readout * readout, axis=-1, keepdims=True))
        grouped = ((readout - mean_v) * lax.rsqrt(square - mean_v * mean_v + group_eps)).reshape(batch_size, full_width)
        grouped = grouped * head_gain[layer_id].astype(jnp.float32)
        gated_rows = (jax.nn.silu(gate_rows) * grouped).astype(jnp.bfloat16)
        hidden_x = (xfloat + jnp.dot(gated_rows, w_out[layer_id], preferred_element_type=jnp.float32)).astype(jnp.bfloat16)
        outputs.append(updated.reshape(batch_size, full_width, DK))
    return (hidden_x, jnp.stack(outputs))
```

```python
import jax
import jax.numpy as jnp
from jax import lax
from jax.sharding import PartitionSpec as P

D = 4096
HEADS = 16
DK = 128
LAYERS = 2


norm_eps = 1e-06
group_eps = 1e-05
rotary_base = 10000.0


def partner_2(value, axis, apart):
    mask = 2**apart
    pairs = [(source, source ^ mask) for source in range(lax.axis_size(axis))]
    return lax.ppermute(value, axis, pairs)


def rotate(values, positions):
    half_size = values.shape[-1] // 2
    inverse = rotary_base ** (-jnp.arange(half_size, dtype=jnp.float32) / half_size)
    angles = positions.astype(jnp.float32)[:, None] * inverse[None, :]
    cosine = jnp.cos(angles)[:, None, :]
    sine_v = jnp.sin(angles)[:, None, :]
    first_part = values[..., :half_size]
    second = values[..., half_size:]
    return jnp.concatenate(
        [first_part * cosine - second * sine_v, first_part * sine_v + second * cosine], axis=-1
    )


def decays(head_ids):
    return 1.0 - jnp.exp2(-1.0 - 9.0 * head_ids.astype(jnp.float32) / (HEADS - 1))


def gather_rows(value, axis):
    return lax.all_gather(value, axis, axis=0, tiled=True)


def sum_rows(partial_value, axis):
    count = lax.axis_size(axis)
    rows = partial_value.shape[0] // count
    split = partial_value.reshape(count, rows, partial_value.shape[1])
    swapped = lax.all_to_all(split, axis, split_axis=0, concat_axis=0, tiled=True)
    return jnp.sum(swapped.astype(jnp.float32), axis=0)


def body(tokens, lengths, states, norm_gain, w_query, w_key, w_value, w_gate, head_gain, w_out):
    tp_index = lax.axis_index("tp")
    columns = w_query.shape[2]
    pieces = max(DK // columns, 1)
    levels = pieces.bit_length() - 1
    local_heads = max(columns // DK, 1)
    value_cols = columns // local_heads
    head_ids = tp_index * columns // DK + jnp.arange(local_heads, dtype=jnp.int32)
    gammas = decays(head_ids)
    hidden_x = tokens
    outputs = []
    for layer_id in range(LAYERS):
        prior_state = states[layer_id]
        row_total = prior_state.shape[0]
        gathered_f = gather_rows(hidden_x, "tp").astype(jnp.float32)
        normed = (gathered_f * norm_gain[layer_id].astype(jnp.float32)).astype(jnp.bfloat16)
        squares = jnp.sum(gathered_f * gathered_f, axis=1, keepdims=True)
        high = squares.astype(jnp.bfloat16)
        low = (squares - high.astype(jnp.float32)).astype(jnp.bfloat16)
        blocks = [
            jnp.dot(normed, w[layer_id], preferred_element_type=jnp.float32).astype(jnp.bfloat16)
            for w in (w_query, w_key, w_value, w_gate)
        ]
        summed = sum_rows(jnp.concatenate(blocks + [high, low], axis=1), "dp")
        own_squares = summed[:, 4 * columns] + summed[:, 4 * columns + 1]
        row_scale = lax.rsqrt(own_squares / D + norm_eps)
        projected = (summed[:, : 4 * columns] * row_scale[:, None]).astype(jnp.bfloat16)
        query_rows = projected[:, :columns]
        key_rows = projected[:, columns : 2 * columns]
        value_rows = projected[:, 2 * columns : 3 * columns]
        gate_rows = projected[:, 3 * columns :]
        stacked = jnp.stack([query_rows, key_rows])
        for join_level_id in range(levels):
            partner = partner_2(stacked, "tp", join_level_id)
            upper_bit = tp_index // 2**join_level_id % 2
            stacked = jnp.where(
                upper_bit == 1,
                jnp.concatenate([partner, stacked], axis=-1),
                jnp.concatenate([stacked, partner], axis=-1),
            )
        query_f = rotate(
            stacked[0].astype(jnp.float32).reshape(row_total, local_heads, DK), lengths
        )
        key_f = rotate(
            stacked[1].astype(jnp.float32).reshape(row_total, local_heads, DK), lengths
        ) * DK ** (-0.5)
        values_f = value_rows.astype(jnp.float32).reshape(row_total, local_heads, value_cols)
        state_view = prior_state.reshape(row_total, local_heads, value_cols, DK)
        updated = gammas[None, :, None, None] * state_view + jnp.einsum(
            "shd,shv->shvd", key_f, values_f
        )
        readout = jnp.einsum("shd,shvd->shv", query_f, updated)
        head_stats = jnp.stack([jnp.sum(readout, axis=-1), jnp.sum(readout * readout, axis=-1)])
        for level_id in range(levels):
            head_stats = head_stats + partner_2(head_stats, "tp", level_id)
        mean_v = head_stats[0][..., None] / DK
        square = head_stats[1][..., None] / DK
        grouped = ((readout - mean_v) * lax.rsqrt(square - mean_v * mean_v + group_eps)).reshape(
            row_total, columns
        )
        grouped = grouped * head_gain[layer_id].astype(jnp.float32)
        gated_rows = (jax.nn.silu(gate_rows.astype(jnp.float32)) * grouped).astype(jnp.bfloat16)
        every_row = gather_rows(gated_rows, "dp")
        branch_parts = jnp.dot(every_row, w_out[layer_id], preferred_element_type=jnp.float32)
        branch = sum_rows(branch_parts.astype(jnp.bfloat16), "tp")
        hidden_x = (hidden_x.astype(jnp.float32) + branch).astype(jnp.bfloat16)
        outputs.append(updated.reshape(row_total, columns, DK))
    return (hidden_x, jnp.stack(outputs))


def solution(mesh):
    placed = (
        P("tp", "dp"),
        P("dp"),
        P(None, "dp", "tp", None),
        P(None, "dp"),
        P(None, "dp", "tp"),
        P(None, "dp", "tp"),
        P(None, "dp", "tp"),
        P(None, "dp", "tp"),
        P(None, "tp"),
        P(None, "tp", "dp"),
    )
    return jax.shard_map(
        body,
        mesh=mesh,
        in_specs=placed,
        out_specs=(P("tp", "dp"), P(None, "dp", "tp", None)),
        check_vma=False,
    )
```

```python
import jax
import jax.numpy as jnp
from jax import lax
from jax.sharding import PartitionSpec as P

D = 4096
HEADS = 16
DK = 128
LAYERS = 2


norm_eps = 1e-06
group_eps = 1e-05
rotary_base = 10000.0


def partner_2(value, axis, apart):
    mask = 2**apart
    pairs = [(source, source ^ mask) for source in range(lax.axis_size(axis))]
    return lax.ppermute(value, axis, pairs)


def rotate(values, positions):
    half_size = values.shape[-1] // 2
    inverse = rotary_base ** (-jnp.arange(half_size, dtype=jnp.float32) / half_size)
    angles = positions.astype(jnp.float32)[:, None] * inverse[None, :]
    cosine = jnp.cos(angles)[:, None, :]
    sine_v = jnp.sin(angles)[:, None, :]
    first_part = values[..., :half_size]
    second = values[..., half_size:]
    return jnp.concatenate(
        [first_part * cosine - second * sine_v, first_part * sine_v + second * cosine], axis=-1
    )


def decays(head_ids):
    return 1.0 - jnp.exp2(-1.0 - 9.0 * head_ids.astype(jnp.float32) / (HEADS - 1))


STAGES = {"tp": (1, 2), "dp": (2, 2)}


def stage_bits(axis):
    left = lax.axis_size(axis).bit_length() - 1
    groups, low = [], 0
    while left > 0:
        pattern = STAGES[axis]
        width = min(pattern[len(groups) % len(pattern)], left)
        groups.append((low, width))
        low, left = low + width, left - width
    return groups


def exchange(value, axis, mask):
    pairs = [(source, source ^ mask) for source in range(lax.axis_size(axis))]
    return lax.ppermute(value, axis, pairs)


def xor_order(blocks, axis, low, width):
    index = lax.axis_index(axis)
    for bit in range(width):
        is_set = index // 2 ** (low + bit) % 2 == 1
        blocks = [
            jnp.where(is_set, blocks[k ^ 2**bit], blocks[k]) for k in range(len(blocks))
        ]
    return blocks


def gather_rows(value, axis):
    for low, width in stage_bits(axis):
        blocks = [value] + [exchange(value, axis, k << low) for k in range(1, 2**width)]
        value = jnp.concatenate(xor_order(blocks, axis, low, width), axis=0)
    return value


def sum_rows(partial_value, axis):
    for low, width in reversed(stage_bits(axis)):
        blocks = jnp.split(partial_value.astype(jnp.bfloat16), 2**width, axis=0)
        blocks = xor_order(blocks, axis, low, width)
        blocks = blocks[:1] + [exchange(blocks[k], axis, k << low) for k in range(1, 2**width)]
        partial_value = sum(block.astype(jnp.float32) for block in blocks)
    return partial_value


def body(tokens, lengths, states, norm_gain, w_query, w_key, w_value, w_gate, head_gain, w_out):
    tp_index = lax.axis_index("tp")
    columns = w_query.shape[2]
    pieces = max(DK // columns, 1)
    levels = pieces.bit_length() - 1
    local_heads = max(columns // DK, 1)
    value_cols = columns // local_heads
    head_ids = tp_index * columns // DK + jnp.arange(local_heads, dtype=jnp.int32)
    gammas = decays(head_ids)
    hidden_x = tokens
    outputs = []
    for layer_id in range(LAYERS):
        prior_state = states[layer_id]
        row_total = prior_state.shape[0]
        gathered_f = gather_rows(hidden_x, "tp").astype(jnp.float32)
        normed = (gathered_f * norm_gain[layer_id].astype(jnp.float32)).astype(jnp.bfloat16)
        squares = jnp.sum(gathered_f * gathered_f, axis=1, keepdims=True)
        high = squares.astype(jnp.bfloat16)
        low = (squares - high.astype(jnp.float32)).astype(jnp.bfloat16)
        blocks = [
            jnp.dot(normed, w[layer_id], preferred_element_type=jnp.float32).astype(jnp.bfloat16)
            for w in (w_query, w_key, w_value, w_gate)
        ]
        summed = sum_rows(jnp.concatenate(blocks + [high, low], axis=1), "dp")
        own_squares = summed[:, 4 * columns] + summed[:, 4 * columns + 1]
        row_scale = lax.rsqrt(own_squares / D + norm_eps)
        projected = (summed[:, : 4 * columns] * row_scale[:, None]).astype(jnp.bfloat16)
        query_rows = projected[:, :columns]
        key_rows = projected[:, columns : 2 * columns]
        value_rows = projected[:, 2 * columns : 3 * columns]
        gate_rows = projected[:, 3 * columns :]
        stacked = jnp.stack([query_rows, key_rows])
        for join_level_id in range(levels):
            partner = partner_2(stacked, "tp", join_level_id)
            upper_bit = tp_index // 2**join_level_id % 2
            stacked = jnp.where(
                upper_bit == 1,
                jnp.concatenate([partner, stacked], axis=-1),
                jnp.concatenate([stacked, partner], axis=-1),
            )
        query_f = rotate(
            stacked[0].astype(jnp.float32).reshape(row_total, local_heads, DK), lengths
        )
        key_f = rotate(
            stacked[1].astype(jnp.float32).reshape(row_total, local_heads, DK), lengths
        ) * DK ** (-0.5)
        values_f = value_rows.astype(jnp.float32).reshape(row_total, local_heads, value_cols)
        state_view = prior_state.reshape(row_total, local_heads, value_cols, DK)
        updated = gammas[None, :, None, None] * state_view + jnp.einsum(
            "shd,shv->shvd", key_f, values_f
        )
        overlap = jnp.sum(query_f * key_f, axis=-1, keepdims=True)
        readout = (
            gammas[None, :, None] * jnp.einsum("shd,shvd->shv", query_f, state_view)
            + overlap * values_f
        )
        head_stats = jnp.stack([jnp.sum(readout, axis=-1), jnp.sum(readout * readout, axis=-1)])
        for level_id in range(levels):
            head_stats = head_stats + partner_2(head_stats, "tp", level_id)
        mean_v = head_stats[0][..., None] / DK
        square = head_stats[1][..., None] / DK
        grouped = ((readout - mean_v) * lax.rsqrt(square - mean_v * mean_v + group_eps)).reshape(
            row_total, columns
        )
        grouped = grouped * head_gain[layer_id].astype(jnp.float32)
        gated_rows = (jax.nn.silu(gate_rows.astype(jnp.float32)) * grouped).astype(jnp.bfloat16)
        every_row = gather_rows(gated_rows, "dp")
        branch_parts = jnp.dot(every_row, w_out[layer_id], preferred_element_type=jnp.float32)
        branch = sum_rows(branch_parts, "tp")
        hidden_x = (hidden_x.astype(jnp.float32) + branch).astype(jnp.bfloat16)
        outputs.append(updated.reshape(row_total, columns, DK))
    return (hidden_x, jnp.stack(outputs))


def solution(mesh):
    placed = (
        P("tp", "dp"),
        P("dp"),
        P(None, "dp", "tp", None),
        P(None, "dp"),
        P(None, "dp", "tp"),
        P(None, "dp", "tp"),
        P(None, "dp", "tp"),
        P(None, "dp", "tp"),
        P(None, "tp"),
        P(None, "tp", "dp"),
    )
    return jax.shard_map(
        body,
        mesh=mesh,
        in_specs=placed,
        out_specs=(P("tp", "dp"), P(None, "dp", "tp", None)),
        check_vma=False,
    )
```

```python
import jax
import jax.numpy as jnp
from jax import lax
from jax.sharding import PartitionSpec as P

D = 4096
HEADS = 16
DK = 128
LAYERS = 2


norm_eps = 1e-06
group_eps = 1e-05
rotary_base = 10000.0


def partner_2(value, axis, apart):
    mask = 2**apart
    pairs = [(source, source ^ mask) for source in range(lax.axis_size(axis))]
    return lax.ppermute(value, axis, pairs)


def rotate(values, positions):
    half_size = values.shape[-1] // 2
    inverse = rotary_base ** (-jnp.arange(half_size, dtype=jnp.float32) / half_size)
    angles = positions.astype(jnp.float32)[:, None] * inverse[None, :]
    cosine = jnp.cos(angles)[:, None, :]
    sine_v = jnp.sin(angles)[:, None, :]
    first_part = values[..., :half_size]
    second = values[..., half_size:]
    return jnp.concatenate(
        [first_part * cosine - second * sine_v, first_part * sine_v + second * cosine], axis=-1
    )


def decays(head_ids):
    return 1.0 - jnp.exp2(-1.0 - 9.0 * head_ids.astype(jnp.float32) / (HEADS - 1))


STAGES = {"tp": (1, 2), "dp": (2, 2)}


def stage_bits(axis):
    left = lax.axis_size(axis).bit_length() - 1
    groups, low = [], 0
    while left > 0:
        pattern = STAGES[axis]
        width = min(pattern[len(groups) % len(pattern)], left)
        groups.append((low, width))
        low, left = low + width, left - width
    return groups


def exchange(value, axis, mask):
    pairs = [(source, source ^ mask) for source in range(lax.axis_size(axis))]
    return lax.ppermute(value, axis, pairs)


def xor_order(blocks, axis, low, width):
    index = lax.axis_index(axis)
    for bit in range(width):
        is_set = index // 2 ** (low + bit) % 2 == 1
        blocks = [
            jnp.where(is_set, blocks[k ^ 2**bit], blocks[k]) for k in range(len(blocks))
        ]
    return blocks


def gather_rows(value, axis, stages):
    for low, width in stages:
        blocks = [value] + [exchange(value, axis, k << low) for k in range(1, 2**width)]
        value = jnp.concatenate(xor_order(blocks, axis, low, width), axis=0)
    return value


def sum_rows(partial_value, axis, stages):
    for low, width in reversed(stages):
        blocks = jnp.split(partial_value.astype(jnp.bfloat16), 2**width, axis=0)
        blocks = xor_order(blocks, axis, low, width)
        blocks = blocks[:1] + [exchange(blocks[k], axis, k << low) for k in range(1, 2**width)]
        partial_value = sum(block.astype(jnp.float32) for block in blocks)
    return partial_value


def sum_shared(partial_value, axis, stages):
    for low, width in stages:
        own = partial_value.astype(jnp.bfloat16)
        others = [exchange(own, axis, k << low) for k in range(1, 2**width)]
        partial_value = sum(block.astype(jnp.float32) for block in [own] + others)
    return partial_value


def body(tokens, lengths, states, norm_gain, w_query, w_key, w_value, w_gate, head_gain, w_out):
    tp_index = lax.axis_index("tp")
    columns = w_query.shape[2]
    pieces = max(DK // columns, 1)
    levels = pieces.bit_length() - 1
    local_heads = max(columns // DK, 1)
    value_cols = columns // local_heads
    head_ids = tp_index * columns // DK + jnp.arange(local_heads, dtype=jnp.int32)
    gammas = decays(head_ids)
    near, far = stage_bits("tp")[:1], stage_bits("tp")[1:]
    over_dp = stage_bits("dp")
    shared_x = gather_rows(tokens, "tp", near)
    outputs = []
    for layer_id in range(LAYERS):
        prior_state = states[layer_id]
        row_total = prior_state.shape[0]
        gathered_f = gather_rows(shared_x, "tp", far).astype(jnp.float32)
        normed = (gathered_f * norm_gain[layer_id].astype(jnp.float32)).astype(jnp.bfloat16)
        squares = jnp.sum(gathered_f * gathered_f, axis=1, keepdims=True)
        high = squares.astype(jnp.bfloat16)
        low = (squares - high.astype(jnp.float32)).astype(jnp.bfloat16)
        blocks = [
            jnp.dot(normed, w[layer_id], preferred_element_type=jnp.float32).astype(jnp.bfloat16)
            for w in (w_query, w_key, w_value, w_gate)
        ]
        summed = sum_rows(jnp.concatenate(blocks + [high, low], axis=1), "dp", over_dp)
        own_squares = summed[:, 4 * columns] + summed[:, 4 * columns + 1]
        row_scale = lax.rsqrt(own_squares / D + norm_eps)
        projected = (summed[:, : 4 * columns] * row_scale[:, None]).astype(jnp.bfloat16)
        query_rows = projected[:, :columns]
        key_rows = projected[:, columns : 2 * columns]
        value_rows = projected[:, 2 * columns : 3 * columns]
        gate_rows = projected[:, 3 * columns :]
        stacked = jnp.stack([query_rows, key_rows])
        for join_level_id in range(levels):
            partner = partner_2(stacked, "tp", join_level_id)
            upper_bit = tp_index // 2**join_level_id % 2
            stacked = jnp.where(
                upper_bit == 1,
                jnp.concatenate([partner, stacked], axis=-1),
                jnp.concatenate([stacked, partner], axis=-1),
            )
        query_f = rotate(
            stacked[0].astype(jnp.float32).reshape(row_total, local_heads, DK), lengths
        )
        key_f = rotate(
            stacked[1].astype(jnp.float32).reshape(row_total, local_heads, DK), lengths
        ) * DK ** (-0.5)
        values_f = value_rows.astype(jnp.float32).reshape(row_total, local_heads, value_cols)
        state_view = prior_state.reshape(row_total, local_heads, value_cols, DK)
        overlap = jnp.sum(query_f * key_f, axis=-1, keepdims=True)
        readout = (
            gammas[None, :, None] * jnp.einsum("shd,shvd->shv", query_f, state_view)
            + overlap * values_f
        )
        head_stats = jnp.stack([jnp.sum(readout, axis=-1), jnp.sum(readout * readout, axis=-1)])
        for level_id in range(levels):
            head_stats = head_stats + partner_2(head_stats, "tp", level_id)
        mean_v = head_stats[0][..., None] / DK
        square = head_stats[1][..., None] / DK
        grouped = ((readout - mean_v) * lax.rsqrt(square - mean_v * mean_v + group_eps)).reshape(
            row_total, columns
        )
        grouped = grouped * head_gain[layer_id].astype(jnp.float32)
        gated_rows = (jax.nn.silu(gate_rows.astype(jnp.float32)) * grouped).astype(jnp.bfloat16)
        every_row = gather_rows(gated_rows, "dp", over_dp)
        branch_parts = jnp.dot(every_row, w_out[layer_id], preferred_element_type=jnp.float32)
        branch = sum_rows(branch_parts, "tp", far)
        if layer_id < LAYERS - 1:
            branch, key_f, states = lax.optimization_barrier((branch, key_f, states))
            branch = sum_shared(branch, "tp", near)
            shared_x = (shared_x.astype(jnp.float32) + branch).astype(jnp.bfloat16)
        else:
            branch = sum_rows(branch, "tp", near)
            for low, width in near:
                shared_x = xor_order(jnp.split(shared_x, 2**width), "tp", low, width)[0]
            hidden_x = (shared_x.astype(jnp.float32) + branch).astype(jnp.bfloat16)
        updated = gammas[None, :, None, None] * state_view + jnp.einsum(
            "shd,shv->shvd", key_f, values_f
        )
        outputs.append(updated.reshape(row_total, columns, DK))
    return (hidden_x, jnp.stack(outputs))


def solution(mesh):
    placed = (
        P("tp", "dp"),
        P("dp"),
        P(None, "dp", "tp", None),
        P(None, "dp"),
        P(None, "dp", "tp"),
        P(None, "dp", "tp"),
        P(None, "dp", "tp"),
        P(None, "dp", "tp"),
        P(None, "tp"),
        P(None, "tp", "dp"),
    )
    return jax.shard_map(
        body,
        mesh=mesh,
        in_specs=placed,
        out_specs=(P("tp", "dp"), P(None, "dp", "tp", None)),
        check_vma=False,
    )
```
